32 devices in a mesh: sp: 8 (over z, core), tp: 4 (over y, x).
Axes of the slice: x: 2, y: 2, z: 4, core: 2. Of those that a mesh axis runs over, the one named last changes fastest.
Arguments:
- target: bfloat16 [1024, 2048], P(('sp', 'tp')), may hold values from -3 to 3
- source: bfloat16 [6144, 2048], P(('sp', 'tp')), may hold values from -6 to 6
- target_gain: float32 [2048], replicated, may hold values from 0.1 to 1.9
- source_gain: float32 [2048], replicated, may hold values from 0.1 to 1.9
- query_weight: bfloat16 [2048, 2048], P(None, 'tp'), may hold values from -0.125 to 0.125
- key_matrix: bfloat16 [2048, 256], replicated, may hold values from -0.125 to 0.125
- value_matrix: bfloat16 [2048, 256], replicated, may hold values from -0.125 to 0.125
- query_gain: float32 [16, 128], P('tp'), may hold values from 0.24 to 20
- key_gain: float32 [2, 128], replicated, may hold values from 1.2 to 4
- out_weight: bfloat16 [2048, 2048], P('tp'), may hold values from -0.125 to 0.125
Outputs:
- updated_target: bfloat16 [1024, 2048], P(('sp', 'tp'))
The draws below stay inside these ranges and needn't reach their ends.
All inputs are finite; a program needn't handle non-finite values.
Results may differ from the reference program's by a relative error of at most 0.018.
The reference program's roundings to bfloat16 on the way count: a program that leaves them out, or rounds other values in their place, can miss the bound.
Values may be sent and summed in bfloat16 or wider, within the bound.
A program may use at most 64 MiB of HBM per device.

```python
import math
import jax
import jax.numpy as jnp
from jax import lax

MODEL_WIDTH = 2048
QUERY_HEAD_COUNT = 16
KEY_VALUE_HEADS = 2
HEAD_SIZE = 128
TARGET_PER_SHARD = 128
TGT = 1024
SOURCE_LENGTH = 6144
N_SP = 8


def draw_query_gain(key, part):
    random_cell_key = jax.random.fold_in(jax.random.fold_in(key, 17), 1)
    return jnp.exp(jax.random.uniform(random_cell_key, (QUERY_HEAD_COUNT, HEAD_SIZE), jnp.float32, math.log(1.2), math.log(2.2)))


def draw_key_gain(key, part):
    random_cell_key = jax.random.fold_in(key, 29)
    return jnp.exp(jax.random.uniform(random_cell_key, (KEY_VALUE_HEADS, HEAD_SIZE), jnp.float32, math.log(1.2), math.log(2.2)))


def steps_of(rng, shape, shards, low, largest):
    def one(axis_at, parts):
        steps = jax.random.uniform(jax.random.fold_in(jax.random.fold_in(rng, 6), axis_at), (parts,), jnp.float32, low / len(shards), largest / len(shards))
        return jnp.repeat(jnp.exp(steps), shape[axis_at] // parts).reshape((-1,) + (1,) * (len(shape) - axis_at - 1))

    level = one(*shards[0])
    for cut in shards[1:]:
        level = level * one(*cut)
    return level


def centred(own_key, extent, width, reach, cuts=(), kind=jnp.bfloat16):
    entries = width * jax.random.normal(own_key, extent, jnp.float32)
    if cuts:
        entries = entries * steps_of(own_key, extent, cuts, -0.22, 0.18)
    return jnp.clip(entries, -reach, reach).astype(kind)


def setup_inputs(seed: int = 0) -> dict:
    seeds = jax.random.split(jax.random.key(seed), 11)
    target = centred(seeds[0], (TGT, MODEL_WIDTH), 0.5, 3.0, ((0, 32),))
    source = centred(seeds[1], (SOURCE_LENGTH, MODEL_WIDTH), 1.0, 6.0, ((0, 32),))
    target_gain = jnp.clip(1.0 + 0.18 * jax.random.normal(seeds[2], (MODEL_WIDTH,), jnp.float32), 0.1, 1.9)
    source_gain = jnp.clip(1.0 + 0.18 * jax.random.normal(seeds[3], (MODEL_WIDTH,), jnp.float32), 0.1, 1.9)
    query_weight = centred(seeds[4], (MODEL_WIDTH, QUERY_HEAD_COUNT * HEAD_SIZE), MODEL_WIDTH ** -0.5, 0.125, ((1, 4),))
    key_matrix = centred(seeds[5], (MODEL_WIDTH, KEY_VALUE_HEADS * HEAD_SIZE), MODEL_WIDTH ** -0.5, 0.125)
    value_matrix = centred(seeds[6], (MODEL_WIDTH, KEY_VALUE_HEADS * HEAD_SIZE), MODEL_WIDTH ** -0.5, 0.125)
    query_gain = draw_query_gain(jax.random.fold_in(seeds[10], 71), 0)
    key_gain = draw_key_gain(jax.random.fold_in(seeds[10], 71), 0)
    out_weight = centred(seeds[9], (QUERY_HEAD_COUNT * HEAD_SIZE, MODEL_WIDTH), (QUERY_HEAD_COUNT * HEAD_SIZE) ** -0.5, 0.125, ((0, 4),))
    return dict(target=target, source=source, target_gain=target_gain, source_gain=source_gain, query_weight=query_weight, key_matrix=key_matrix, value_matrix=value_matrix, query_gain=query_gain, key_gain=key_gain, out_weight=out_weight)


EPSILON = 1e-06

def normed(values_in, gain):
    return values_in * lax.rsqrt(lax.optimization_barrier(jnp.mean(values_in * values_in, axis=-1, keepdims=True)) + EPSILON) * gain

def reference(target, source, target_gain, source_gain, query_weight, key_matrix, value_matrix, query_gain, key_gain, out_weight):
    normed_source_rows = normed(source.astype(jnp.float32), source_gain).astype(jnp.bfloat16)
    unnormed_keys = jnp.dot(normed_source_rows, key_matrix, preferred_element_type=jnp.float32).reshape(SOURCE_LENGTH, KEY_VALUE_HEADS, HEAD_SIZE)
    key_rows = normed(unnormed_keys, key_gain).astype(jnp.bfloat16)
    value_vectors = jnp.dot(normed_source_rows, value_matrix, preferred_element_type=jnp.float32).astype(jnp.bfloat16).reshape(SOURCE_LENGTH, KEY_VALUE_HEADS, HEAD_SIZE)
    target_normed = normed(target.astype(jnp.float32), target_gain).astype(jnp.bfloat16)
    raw_queries = jnp.dot(target_normed, query_weight, preferred_element_type=jnp.float32).reshape(TGT, QUERY_HEAD_COUNT, HEAD_SIZE)
    query_vectors = normed(raw_queries, query_gain).astype(jnp.bfloat16)
    heads_per_group = QUERY_HEAD_COUNT // KEY_VALUE_HEADS
    query_tiles = query_vectors.reshape(N_SP, TARGET_PER_SHARD, KEY_VALUE_HEADS, heads_per_group, HEAD_SIZE)
    key_float = key_rows.astype(jnp.float32)
    value_float = value_vectors.astype(jnp.float32)
    score_scale = 1.0 / math.sqrt(HEAD_SIZE)

    def by_block(query_block):
        scores = jnp.einsum('rgqd,ngd->rgqn', query_block.astype(jnp.float32), key_float) * score_scale
        maxima = lax.optimization_barrier(jnp.max(scores, axis=-1, keepdims=True))
        weights = jnp.exp(scores - maxima)
        totals = lax.optimization_barrier(jnp.sum(weights, axis=-1))
        shares = lax.optimization_barrier(weights.astype(jnp.bfloat16)).astype(jnp.float32)
        summed = jnp.einsum('rgqn,ngd->rgqd', shares, value_float)
        return (summed / totals[..., None]).astype(jnp.bfloat16)
    attended = lax.map(by_block, query_tiles).reshape(TGT, QUERY_HEAD_COUNT * HEAD_SIZE)
    update = jnp.dot(attended, out_weight, preferred_element_type=jnp.float32)
    return (target.astype(jnp.float32) + update).astype(jnp.bfloat16)
```

```python
import functools
import math

import jax
import jax.numpy as jnp
from jax import lax
from jax.experimental import pallas as pl
from jax.experimental.pallas import tpu as pltpu
from jax.sharding import PartitionSpec as P

KEY_VALUE_HEADS = 2
HEAD_SIZE = 128


EPSILON = 1e-06


def normed(values_in, gain):
    return (
        values_in
        * lax.rsqrt(jnp.mean(values_in * values_in, axis=-1, keepdims=True) + EPSILON)
        * gain
    )


def softmax_step(running, scores, seg_values, form):
    maxima, totals, weighted = running
    new_maxima = jnp.maximum(maxima, jnp.max(scores, axis=-1))
    fading = jnp.exp(maxima - new_maxima)
    weights = jnp.exp(scores - new_maxima[..., None])
    totals = totals * fading + jnp.sum(weights, axis=-1)
    weighted = weighted * fading[..., None] + jnp.einsum(
        form, weights.astype(jnp.bfloat16), seg_values, preferred_element_type=jnp.float32
    )
    return (new_maxima, totals, weighted)


def in_blocks(advance, running, segment, own_rows, limit):
    length = segment[0].shape[0]
    shards = length // own_rows
    widest = max(own_rows, limit)
    per_block = max(
        [
            number
            for number in range(1, shards + 1)
            if shards % number == 0 and own_rows * number <= widest
        ]
    )
    blocks = shards // per_block
    shaped = tuple(
        (member.reshape((blocks, own_rows * per_block) + member.shape[1:]) for member in segment)
    )

    def one_turn(carried, portion):
        return (advance(carried, portion), None)

    return lax.scan(one_turn, running, shaped)[0]


def body(
    target,
    source,
    target_gain,
    source_gain,
    query_weight,
    key_matrix,
    value_matrix,
    query_gain,
    key_gain,
    out_weight,
):
    local_heads = query_weight.shape[1] // HEAD_SIZE
    score_scale = 1.0 / math.sqrt(HEAD_SIZE)
    target_normed = normed(target.astype(jnp.float32), target_gain).astype(jnp.bfloat16)
    segment = lax.all_gather(target_normed, "tp", axis=0, tiled=True)
    raw_queries = jnp.dot(segment, query_weight, preferred_element_type=jnp.float32)
    shaped = raw_queries.reshape(segment.shape[0], local_heads, HEAD_SIZE)
    query_vectors = normed(shaped, query_gain).astype(jnp.bfloat16)
    block_rows = query_vectors.shape[0]
    normed_source_rows = normed(source.astype(jnp.float32), source_gain).astype(jnp.bfloat16)
    unnormed_keys = jnp.dot(
        normed_source_rows, key_matrix, preferred_element_type=jnp.float32
    ).reshape(source.shape[0], KEY_VALUE_HEADS, HEAD_SIZE)
    key_rows = normed(unnormed_keys, key_gain).astype(jnp.bfloat16)
    value_vectors = (
        jnp.dot(normed_source_rows, value_matrix, preferred_element_type=jnp.float32)
        .astype(jnp.bfloat16)
        .reshape(source.shape[0], KEY_VALUE_HEADS, HEAD_SIZE)
    )
    each_head_view = lax.axis_size("tp") // KEY_VALUE_HEADS
    sent_keys = jnp.repeat(key_rows, each_head_view, axis=1)
    sent_values = jnp.repeat(value_vectors, each_head_view, axis=1)
    head_keys, head_values = (
        lax.all_to_all(sent_keys, "tp", split_axis=1, concat_axis=0, tiled=True),
        lax.all_to_all(sent_values, "tp", split_axis=1, concat_axis=0, tiled=True),
    )
    head_keys = head_keys.reshape(-1, HEAD_SIZE)
    head_values = head_values.reshape(-1, HEAD_SIZE)
    own_rows = head_keys.shape[0]
    small_shape = (block_rows, local_heads)
    initial = (
        jnp.full(small_shape, -1e30, jnp.float32),
        jnp.zeros(small_shape, jnp.float32),
        jnp.zeros(small_shape + (HEAD_SIZE,), jnp.float32),
    )

    def advance(carried, portion):
        scores = (
            jnp.einsum("rhd,nd->rhn", query_vectors, portion[0], preferred_element_type=jnp.float32)
            * score_scale
        )
        return softmax_step(carried, scores, portion[1], "rhn,nd->rhd")

    maxima, totals, weighted = in_blocks(
        advance,
        initial,
        (
            lax.all_gather(head_keys, "sp", axis=0, tiled=True),
            lax.all_gather(head_values, "sp", axis=0, tiled=True),
        ),
        own_rows,
        1024,
    )
    attended = (
        (weighted / totals[..., None])
        .astype(jnp.bfloat16)
        .reshape(block_rows, local_heads * HEAD_SIZE)
    )
    portion = attended
    update = lax.psum_scatter(
        jnp.dot(portion, out_weight, preferred_element_type=jnp.float32).astype(jnp.bfloat16),
        "tp",
        scatter_dimension=0,
        tiled=True,
    ).astype(jnp.float32)
    return (target.astype(jnp.float32) + update).astype(jnp.bfloat16)


MESH = pl.DeviceIdType.MESH
CORES = 2


def fused_kernel(
    n_sp,
    n_tp,
    target_hbm,
    source_hbm,
    target_gain,
    source_gain,
    query_hbm,
    key_hbm,
    value_hbm,
    query_gain,
    key_gain,
    out_hbm,
    update,
    target_in,
    source_in,
    query_w,
    key_w,
    value_w,
    out_w,
    targets,
    queries,
    pairs,
    foreign,
    maxima,
    totals,
    weighted,
    outgoing,
    incoming,
    load_sem,
    target_send,
    target_recv,
    z_send,
    z_recv,
    y_send,
    y_recv,
    x_send,
    x_recv,
    d_send,
    d_recv,
    out_send,
    out_recv,
):
    planes = n_sp // CORES
    sp = lax.axis_index("sp")
    tp = lax.axis_index("tp")
    z, core = sp // CORES, sp % CORES
    y, x = tp // 2, tp % 2
    tp_x = y * 2 + (1 - x)
    tp_y = (1 - y) * 2 + x
    tp_xy = (1 - y) * 2 + (1 - x)
    mate = z * CORES + (1 - core)
    above, below = sp + CORES, sp - CORES
    head = HEAD_SIZE
    rows_t = target_in.shape[0]
    rows_s = source_in.shape[0]
    heads = query_gain.shape[0]
    rows_q = n_tp * rows_t

    loads = [
        pltpu.make_async_copy(a, b, load_sem.at[n])
        for n, (a, b) in enumerate(
            (
                (target_hbm, target_in),
                (source_hbm, source_in),
                (key_hbm, key_w),
                (value_hbm, value_w),
                (query_hbm, query_w),
                (out_hbm, out_w),
            )
        )
    ]
    for load in loads:
        load.start()

    barrier = pltpu.get_barrier_semaphore()
    for peer in ((sp, tp_x), (sp, tp_y), (sp, tp_xy), (mate, tp)):
        pl.semaphore_signal(barrier, inc=1, device_id=peer, device_id_type=MESH)

    @pl.when(z > 0)
    def _():
        pl.semaphore_signal(barrier, inc=1, device_id=(below, tp), device_id_type=MESH)

    @pl.when(z < planes - 1)
    def _():
        pl.semaphore_signal(barrier, inc=1, device_id=(above, tp), device_id_type=MESH)

    def remote(src, dst, send, recv, peer):
        return pltpu.make_async_remote_copy(
            src_ref=src,
            dst_ref=dst,
            send_sem=send,
            recv_sem=recv,
            device_id=peer,
            device_id_type=MESH,
        )

    loads[0].wait()
    targets[tp] = normed(target_in[...].astype(jnp.float32), target_gain[...]).astype(jnp.bfloat16)

    pl.semaphore_wait(barrier, 4 + jnp.minimum(z, 1) + jnp.minimum(planes - 1 - z, 1))

    def target_copy(slot, n, peer):
        return remote(
            targets.at[slot], targets.at[slot], target_send.at[n], target_recv.at[n], peer
        )

    target_x = target_copy(tp, 0, (sp, tp_x))
    target_y = target_copy(tp, 1, (sp, tp_y))
    target_relay = target_copy(tp_x, 2, (sp, tp_y))
    target_x.start()
    target_y.start()

    loads[1].wait()
    source_normed = normed(source_in[...].astype(jnp.float32), source_gain[...]).astype(
        jnp.bfloat16
    )
    loads[2].wait()
    raw_keys = jnp.dot(source_normed, key_w[...], preferred_element_type=jnp.float32)
    loads[3].wait()
    raw_values = jnp.dot(source_normed, value_w[...], preferred_element_type=jnp.float32)

    made = []
    for h in range(KEY_VALUE_HEADS):
        cut = slice(h * head, (h + 1) * head)
        keys = normed(raw_keys[:, cut], key_gain[h : h + 1, :]).astype(jnp.bfloat16)
        made.append((keys, raw_values[:, cut].astype(jnp.bfloat16)))
    mine_zero = y == 0
    for part in range(2):
        cut = slice(part * head, (part + 1) * head)
        pairs[z, tp, core, :, cut] = jnp.where(mine_zero, made[0][part], made[1][part])
        foreign[z, :, cut] = jnp.where(mine_zero, made[1][part], made[0][part])

    def z_copies(at, up):
        peer = (above if up else below, tp)
        own = pairs.at[at, tp, core]
        other = foreign.at[at]
        way = 0 if up else 1
        return (
            remote(own, own, z_send.at[0, way, at], z_recv.at[0, at], peer),
            remote(other, other, z_send.at[1, way, at], z_recv.at[1, at], peer),
        )

    def along_z(at, act):
        @pl.when(jnp.logical_and(at <= z, z < planes - 1))
        def _():
            for copy in z_copies(at, True):
                act(copy)

        @pl.when(jnp.logical_and(at >= z, z > 0))
        def _():
            for copy in z_copies(at, False):
                act(copy)

    def y_copy(at):
        return remote(
            foreign.at[at], pairs.at[at, tp, core], y_send.at[at], y_recv.at[at], (sp, tp_y)
        )

    def y_arrival(at):
        return remote(
            foreign.at[at], pairs.at[at, tp_y, core], y_send.at[at], y_recv.at[at], (sp, tp_y)
        )

    def x_copy(at, n, slot):
        block = pairs.at[at, slot, core]
        return remote(block, block, x_send.at[n, at], x_recv.at[n, at], (sp, tp_x))

    slots = (tp, tp_y, tp_x, tp_xy)

    def d_copy(at, n):
        block = pairs.at[at, slots[n], core]
        return remote(block, block, d_send.at[n, at], d_recv.at[n, at], (mate, tp))

    def d_arrival(at, n):
        block = pairs.at[at, slots[n], 1 - core]
        return remote(block, block, d_send.at[n, at], d_recv.at[n, at], (mate, tp))

    def place(turn):
        other = planes - 1 - z
        near = jnp.minimum(z, other)
        step = (turn + 1) // 2
        signed = z + step * (1 - 2 * (turn % 2))
        far = jnp.where(z < other, turn, planes - 1 - turn)
        return jnp.where(turn <= 2 * near, signed, far)

    def launch(at):
        along_z(at, lambda copy: copy.start())
        x_copy(at, 0, tp).start()
        y_copy(at).start()
        d_copy(at, 0).start()

    def relay_y(at):
        y_arrival(at).wait_recv()
        x_copy(at, 1, tp_y).start()
        d_copy(at, 1).start()

    def take_x(at):
        x_copy(at, 0, tp_x).wait_recv()
        d_copy(at, 2).start()
        x_copy(at, 1, tp_xy).wait_recv()
        d_copy(at, 3).start()

    scale = math.log2(math.e) / math.sqrt(head)

    def attend(at, n):
        d_arrival(at, n).wait_recv()
        both = pairs[at, slots[n]].reshape(CORES * rows_s, 2 * head)
        scores = lax.dot_general(
            both[:, :head],
            queries[...],
            (((1,), (1,)), ((), ())),
            preferred_element_type=jnp.float32,
        )
        before = maxima[...]
        after = jnp.maximum(before, jnp.max(scores, axis=0, keepdims=True))
        weights = jnp.exp2((scores - after) * scale)
        fading = jnp.exp2((before - after) * scale)
        maxima[...] = after
        totals[...] = totals[...] * fading + jnp.sum(weights, axis=0, keepdims=True)
        weighted[...] = weighted[...] * fading + lax.dot_general(
            both[:, head:],
            weights.astype(jnp.bfloat16),
            (((0,), (0,)), ((), ())),
            preferred_element_type=jnp.float32,
        )

    launch(z)

    maxima[...] = jnp.full(maxima.shape, -1e30, jnp.float32)
    totals[...] = jnp.zeros(totals.shape, jnp.float32)
    weighted[...] = jnp.zeros(weighted.shape, jnp.float32)

    target_copy(tp_x, 0, (sp, tp_x)).wait_recv()
    target_relay.start()
    target_copy(tp_y, 1, (sp, tp_y)).wait_recv()
    relay_y(z)
    target_copy(tp_xy, 2, (sp, tp_y)).wait_recv()
    loads[4].wait()
    all_targets = targets[...].reshape(rows_q, targets.shape[2])
    raw = jnp.dot(all_targets, query_w[...], preferred_element_type=jnp.float32)
    for h in range(heads):
        queries[h * rows_q : (h + 1) * rows_q, :] = normed(
            raw[:, h * head : (h + 1) * head], query_gain[h : h + 1, :]
        ).astype(jnp.bfloat16)

    def one_turn(turn, carried):
        at = place(turn)
        prior = place(turn - 1)
        for part in range(2):
            z_copies(at, True)[part].wait_recv()
        launch(at)
        take_x(prior)
        attend(prior, 0)
        attend(prior, 1)
        relay_y(at)
        attend(prior, 2)
        attend(prior, 3)
        return carried

    lax.fori_loop(1, planes, one_turn, 0)
    last = place(planes - 1)
    attend(last, 0)
    attend(last, 1)
    take_x(last)
    attend(last, 2)
    attend(last, 3)

    shared = weighted[...] / totals[...]
    attended = jnp.concatenate(
        [shared[:, h * rows_q : (h + 1) * rows_q].T for h in range(heads)], axis=1
    ).astype(jnp.bfloat16)
    loads[5].wait()
    held = queries
    for h in range(heads):
        held[h * rows_q : (h + 1) * rows_q, :] = attended[:, h * head : (h + 1) * head]

    def product(slot):
        rows = jnp.concatenate(
            [
                held[pl.ds(pl.multiple_of(h * rows_q + slot * rows_t, rows_t), rows_t), :]
                for h in range(heads)
            ],
            axis=1,
        )
        return jnp.dot(rows, out_w[...], preferred_element_type=jnp.float32)

    sends = []
    for n, peer in enumerate((tp_xy, tp_x, tp_y)):
        outgoing[n] = product(peer).astype(jnp.bfloat16)
        copy = remote(outgoing.at[n], incoming.at[n], out_send.at[n], out_recv.at[n], (sp, peer))
        copy.start()
        sends.append(copy)
    mine = product(tp)
    for copy in (target_x, target_y, target_relay):
        copy.wait_send()

    def drain(at, carried):
        along_z(at, lambda copy: copy.wait_send())
        y_copy(at).wait_send()
        x_copy(at, 0, tp).wait_send()
        x_copy(at, 1, tp_y).wait_send()
        for n in range(4):
            d_copy(at, n).wait_send()
        return carried

    lax.fori_loop(0, planes, drain, 0)
    for copy in sends:
        copy.wait_recv()
    update[...] = mine + (
        incoming[0].astype(jnp.float32)
        + incoming[1].astype(jnp.float32)
        + incoming[2].astype(jnp.float32)
    )
    for copy in sends:
        copy.wait_send()


def fused_body(
    n_sp,
    n_tp,
    target,
    source,
    target_gain,
    source_gain,
    query_weight,
    key_matrix,
    value_matrix,
    query_gain,
    key_gain,
    out_weight,
):
    rows_t, width = target.shape
    rows_s = source.shape[0]
    planes = n_sp // CORES
    heads = query_gain.shape[0]
    lanes = heads * n_tp * rows_t
    bf16, f32 = jnp.bfloat16, jnp.float32
    dma = pltpu.SemaphoreType.DMA
    any_spec = pl.BlockSpec(memory_space=pl.ANY)
    vmem_spec = pl.BlockSpec(memory_space=pltpu.VMEM)
    update = pl.pallas_call(
        functools.partial(fused_kernel, n_sp, n_tp),
        out_shape=jax.ShapeDtypeStruct((rows_t, width), f32),
        in_specs=[
            any_spec,
            any_spec,
            vmem_spec,
            vmem_spec,
            any_spec,
            any_spec,
            any_spec,
            vmem_spec,
            vmem_spec,
            any_spec,
        ],
        out_specs=vmem_spec,
        scratch_shapes=[
            pltpu.VMEM(target.shape, bf16),
            pltpu.VMEM(source.shape, bf16),
            pltpu.VMEM(query_weight.shape, bf16),
            pltpu.VMEM(key_matrix.shape, bf16),
            pltpu.VMEM(value_matrix.shape, bf16),
            pltpu.VMEM(out_weight.shape, bf16),
            pltpu.VMEM((n_tp, rows_t, width), bf16),
            pltpu.VMEM((lanes, HEAD_SIZE), bf16),
            pltpu.VMEM((planes, n_tp, CORES, rows_s, 2 * HEAD_SIZE), bf16),
            pltpu.VMEM((planes, rows_s, 2 * HEAD_SIZE), bf16),
            pltpu.VMEM((1, lanes), f32),
            pltpu.VMEM((1, lanes), f32),
            pltpu.VMEM((HEAD_SIZE, lanes), f32),
            pltpu.VMEM((3, rows_t, width), bf16),
            pltpu.VMEM((3, rows_t, width), bf16),
            dma((6,)),
            dma((3,)),
            dma((3,)),
            dma((2, 2, planes)),
            dma((2, planes)),
            dma((planes,)),
            dma((planes,)),
            dma((2, planes)),
            dma((2, planes)),
            dma((4, planes)),
            dma((4, planes)),
            dma((3,)),
            dma((3,)),
        ],
        compiler_params=pltpu.CompilerParams(collective_id=0, has_side_effects=True),
    )(
        target,
        source,
        target_gain.reshape(1, -1),
        source_gain.reshape(1, -1),
        query_weight,
        key_matrix,
        value_matrix,
        query_gain,
        key_gain,
        out_weight,
    )
    return (target.astype(f32) + update).astype(bf16)


def solution(mesh):
    sp, tp = mesh.shape["sp"], mesh.shape["tp"]
    fits = tp == 2 * KEY_VALUE_HEADS and sp % 2 == 0
    return jax.shard_map(
        functools.partial(fused_body, sp, tp) if fits else body,
        mesh=mesh,
        in_specs=(
            P(("sp", "tp"), None),
            P(("sp", "tp"), None),
            P(),
            P(),
            P(None, "tp"),
            P(),
            P(),
            P("tp", None),
            P(),
            P("tp", None),
        ),
        out_specs=P(("sp", "tp"), None),
        check_vma=False,
    )
```

```python
import functools
import math

import jax
import jax.numpy as jnp
from jax import lax
from jax.experimental import pallas as pl
from jax.experimental.pallas import tpu as pltpu
from jax.sharding import PartitionSpec as P

KEY_VALUE_HEADS = 2
HEAD_SIZE = 128


EPSILON = 1e-06


def normed(values_in, gain):
    return (
        values_in
        * lax.rsqrt(jnp.mean(values_in * values_in, axis=-1, keepdims=True) + EPSILON)
        * gain
    )


def softmax_step(running, scores, seg_values, form):
    maxima, totals, weighted = running
    new_maxima = jnp.maximum(maxima, jnp.max(scores, axis=-1))
    fading = jnp.exp(maxima - new_maxima)
    weights = jnp.exp(scores - new_maxima[..., None])
    totals = totals * fading + jnp.sum(weights, axis=-1)
    weighted = weighted * fading[..., None] + jnp.einsum(
        form, weights.astype(jnp.bfloat16), seg_values, preferred_element_type=jnp.float32
    )
    return (new_maxima, totals, weighted)


def in_blocks(advance, running, segment, own_rows, limit):
    length = segment[0].shape[0]
    shards = length // own_rows
    widest = max(own_rows, limit)
    per_block = max(
        [
            number
            for number in range(1, shards + 1)
            if shards % number == 0 and own_rows * number <= widest
        ]
    )
    blocks = shards // per_block
    shaped = tuple(
        (member.reshape((blocks, own_rows * per_block) + member.shape[1:]) for member in segment)
    )

    def one_turn(carried, portion):
        return (advance(carried, portion), None)

    return lax.scan(one_turn, running, shaped)[0]


def body(
    target,
    source,
    target_gain,
    source_gain,
    query_weight,
    key_matrix,
    value_matrix,
    query_gain,
    key_gain,
    out_weight,
):
    local_heads = query_weight.shape[1] // HEAD_SIZE
    score_scale = 1.0 / math.sqrt(HEAD_SIZE)
    target_normed = normed(target.astype(jnp.float32), target_gain).astype(jnp.bfloat16)
    segment = lax.all_gather(target_normed, "tp", axis=0, tiled=True)
    raw_queries = jnp.dot(segment, query_weight, preferred_element_type=jnp.float32)
    shaped = raw_queries.reshape(segment.shape[0], local_heads, HEAD_SIZE)
    query_vectors = normed(shaped, query_gain).astype(jnp.bfloat16)
    block_rows = query_vectors.shape[0]
    normed_source_rows = normed(source.astype(jnp.float32), source_gain).astype(jnp.bfloat16)
    unnormed_keys = jnp.dot(
        normed_source_rows, key_matrix, preferred_element_type=jnp.float32
    ).reshape(source.shape[0], KEY_VALUE_HEADS, HEAD_SIZE)
    key_rows = normed(unnormed_keys, key_gain).astype(jnp.bfloat16)
    value_vectors = (
        jnp.dot(normed_source_rows, value_matrix, preferred_element_type=jnp.float32)
        .astype(jnp.bfloat16)
        .reshape(source.shape[0], KEY_VALUE_HEADS, HEAD_SIZE)
    )
    each_head_view = lax.axis_size("tp") // KEY_VALUE_HEADS
    sent_keys = jnp.repeat(key_rows, each_head_view, axis=1)
    sent_values = jnp.repeat(value_vectors, each_head_view, axis=1)
    head_keys, head_values = (
        lax.all_to_all(sent_keys, "tp", split_axis=1, concat_axis=0, tiled=True),
        lax.all_to_all(sent_values, "tp", split_axis=1, concat_axis=0, tiled=True),
    )
    head_keys = head_keys.reshape(-1, HEAD_SIZE)
    head_values = head_values.reshape(-1, HEAD_SIZE)
    own_rows = head_keys.shape[0]
    small_shape = (block_rows, local_heads)
    initial = (
        jnp.full(small_shape, -1e30, jnp.float32),
        jnp.zeros(small_shape, jnp.float32),
        jnp.zeros(small_shape + (HEAD_SIZE,), jnp.float32),
    )

    def advance(carried, portion):
        scores = (
            jnp.einsum("rhd,nd->rhn", query_vectors, portion[0], preferred_element_type=jnp.float32)
            * score_scale
        )
        return softmax_step(carried, scores, portion[1], "rhn,nd->rhd")

    maxima, totals, weighted = in_blocks(
        advance,
        initial,
        (
            lax.all_gather(head_keys, "sp", axis=0, tiled=True),
            lax.all_gather(head_values, "sp", axis=0, tiled=True),
        ),
        own_rows,
        1024,
    )
    attended = (
        (weighted / totals[..., None])
        .astype(jnp.bfloat16)
        .reshape(block_rows, local_heads * HEAD_SIZE)
    )
    portion = attended
    update = lax.psum_scatter(
        jnp.dot(portion, out_weight, preferred_element_type=jnp.float32).astype(jnp.bfloat16),
        "tp",
        scatter_dimension=0,
        tiled=True,
    ).astype(jnp.float32)
    return (target.astype(jnp.float32) + update).astype(jnp.bfloat16)


MESH = pl.DeviceIdType.MESH
CORES = 2


def fused_kernel(
    n_sp,
    n_tp,
    target_hbm,
    source_hbm,
    target_gain,
    source_gain,
    query_hbm,
    key_hbm,
    value_hbm,
    query_gain,
    key_gain,
    out_hbm,
    update,
    target_in,
    source_in,
    query_w,
    key_w,
    value_w,
    out_w,
    targets,
    queries,
    pairs,
    foreign,
    maxima,
    totals,
    weighted,
    held,
    part_out,
    part_in,
    stats_out,
    stats_in,
    outgoing,
    incoming,
    load_sem,
    target_send,
    target_recv,
    z_send,
    z_recv,
    y_send,
    y_recv,
    x_send,
    x_recv,
    d_send,
    d_recv,
    out_send,
    out_recv,
):
    planes = n_sp // CORES
    sp = lax.axis_index("sp")
    tp = lax.axis_index("tp")
    z, core = sp // CORES, sp % CORES
    y, x = tp // 2, tp % 2
    tp_x = y * 2 + (1 - x)
    tp_y = (1 - y) * 2 + x
    tp_xy = (1 - y) * 2 + (1 - x)
    mate = z * CORES + (1 - core)
    above, below = sp + CORES, sp - CORES
    head = HEAD_SIZE
    rows_t = target_in.shape[0]
    rows_s = source_in.shape[0]
    heads = query_gain.shape[0]
    rows_q = n_tp * rows_t

    loads = [
        pltpu.make_async_copy(a, b, load_sem.at[n])
        for n, (a, b) in enumerate(
            (
                (target_hbm, target_in),
                (source_hbm, source_in),
                (key_hbm, key_w),
                (value_hbm, value_w),
                (query_hbm, query_w),
                (out_hbm, out_w),
            )
        )
    ]
    for load in loads:
        load.start()

    barrier = pltpu.get_barrier_semaphore()
    for peer in ((sp, tp_x), (sp, tp_y), (sp, tp_xy), (mate, tp)):
        pl.semaphore_signal(barrier, inc=1, device_id=peer, device_id_type=MESH)

    @pl.when(z > 0)
    def _():
        pl.semaphore_signal(barrier, inc=1, device_id=(below, tp), device_id_type=MESH)

    @pl.when(z < planes - 1)
    def _():
        pl.semaphore_signal(barrier, inc=1, device_id=(above, tp), device_id_type=MESH)

    def remote(src, dst, send, recv, peer):
        return pltpu.make_async_remote_copy(
            src_ref=src,
            dst_ref=dst,
            send_sem=send,
            recv_sem=recv,
            device_id=peer,
            device_id_type=MESH,
        )

    loads[0].wait()
    targets[tp] = normed(target_in[...].astype(jnp.float32), target_gain[...]).astype(jnp.bfloat16)

    pl.semaphore_wait(barrier, 4 + jnp.minimum(z, 1) + jnp.minimum(planes - 1 - z, 1))

    def target_copy(slot, n, peer):
        return remote(
            targets.at[slot], targets.at[slot], target_send.at[n], target_recv.at[n], peer
        )

    target_x = target_copy(tp, 0, (sp, tp_x))
    target_y = target_copy(tp, 1, (sp, tp_y))
    target_relay = target_copy(tp_x, 2, (sp, tp_y))
    target_x.start()
    target_y.start()

    loads[1].wait()
    source_normed = normed(source_in[...].astype(jnp.float32), source_gain[...]).astype(
        jnp.bfloat16
    )
    loads[2].wait()
    raw_keys = jnp.dot(source_normed, key_w[...], preferred_element_type=jnp.float32)
    loads[3].wait()
    raw_values = jnp.dot(source_normed, value_w[...], preferred_element_type=jnp.float32)

    made = []
    for h in range(KEY_VALUE_HEADS):
        cut = slice(h * head, (h + 1) * head)
        keys = normed(raw_keys[:, cut], key_gain[h : h + 1, :]).astype(jnp.bfloat16)
        made.append((keys, raw_values[:, cut].astype(jnp.bfloat16)))
    mine_zero = y == 0
    for part in range(2):
        cut = slice(part * head, (part + 1) * head)
        pairs[z, tp, core, :, cut] = jnp.where(mine_zero, made[0][part], made[1][part])
        foreign[:, cut] = jnp.where(mine_zero, made[1][part], made[0][part])

    def z_copy(at, n, up):
        block = pairs.at[at, slots[n], core]
        way = 0 if up else 1
        peer = (above if up else below, tp)
        return remote(block, block, z_send.at[n, way, at], z_recv.at[n, at], peer)

    def along_z(at, n, act):
        @pl.when(jnp.logical_and(at <= z, z < planes - 1))
        def _():
            act(z_copy(at, n, True))

        @pl.when(jnp.logical_and(at >= z, z > 0))
        def _():
            act(z_copy(at, n, False))

    def y_copy(slot):
        return remote(foreign, pairs.at[z, slot, core], y_send.at[0], y_recv.at[0], (sp, tp_y))

    def x_copy(src, dst, n):
        return remote(src, dst, x_send.at[n], x_recv.at[n], (sp, tp_x))

    query_copy = x_copy(queries.at[0], queries.at[1], 0)
    part_copy = x_copy(part_out, part_in, 1)
    stats_copy = x_copy(stats_out, stats_in, 2)
    slots = (tp, tp_y)

    def d_copy(at, n):
        block = pairs.at[at, slots[n], core]
        return remote(block, block, d_send.at[n, at], d_recv.at[n, at], (mate, tp))

    def d_arrival(at, n):
        block = pairs.at[at, slots[n], 1 - core]
        return remote(block, block, d_send.at[n, at], d_recv.at[n, at], (mate, tp))

    def place(turn):
        other = planes - 1 - z
        near = jnp.minimum(z, other)
        step = (turn + 1) // 2
        signed = z + step * (1 - 2 * (turn % 2))
        far = jnp.where(z < other, turn, planes - 1 - turn)
        return jnp.where(turn <= 2 * near, signed, far)

    def launch(at, n):
        along_z(at, n, lambda copy: copy.start())
        d_copy(at, n).start()

    def take_z(at, n):
        z_copy(at, n, True).wait_recv()
        launch(at, n)

    scale = math.log2(math.e) / math.sqrt(head)

    def ready(at, n):
        d_arrival(at, n).wait_recv()

    def attend(at, n, half):
        both = pairs[at, slots[n]].reshape(CORES * rows_s, 2 * head)
        scores = lax.dot_general(
            both[:, :head],
            queries[half],
            (((1,), (1,)), ((), ())),
            preferred_element_type=jnp.float32,
        )
        before = maxima[half]
        after = jnp.maximum(before, jnp.max(scores, axis=0, keepdims=True))
        weights = jnp.exp2((scores - after) * scale)
        fading = jnp.exp2((before - after) * scale)
        maxima[half] = after
        totals[half] = totals[half] * fading + jnp.sum(weights, axis=0, keepdims=True)
        weighted[half] = weighted[half] * fading + lax.dot_general(
            both[:, head:],
            weights.astype(jnp.bfloat16),
            (((0,), (0,)), ((), ())),
            preferred_element_type=jnp.float32,
        )

    y_copy(tp).start()
    launch(z, 0)

    maxima[...] = jnp.full(maxima.shape, -1e30, jnp.float32)
    totals[...] = jnp.zeros(totals.shape, jnp.float32)
    weighted[...] = jnp.zeros(weighted.shape, jnp.float32)

    target_copy(tp_x, 0, (sp, tp_x)).wait_recv()
    target_relay.start()
    target_copy(tp_y, 1, (sp, tp_y)).wait_recv()
    y_copy(tp_y).wait_recv()
    launch(z, 1)
    target_copy(tp_xy, 2, (sp, tp_y)).wait_recv()
    loads[4].wait()
    all_targets = targets[...].reshape(rows_q, targets.shape[2])
    raw = jnp.dot(all_targets, query_w[...], preferred_element_type=jnp.float32)
    for h in range(heads):
        queries[0, h * rows_q : (h + 1) * rows_q, :] = normed(
            raw[:, h * head : (h + 1) * head], query_gain[h : h + 1, :]
        ).astype(jnp.bfloat16)

    query_copy.start()

    def one_turn(turn, carried):
        at = place(turn)
        prior = place(turn - 1)
        take_z(at, 0)
        ready(prior, 0)
        attend(prior, 0, 0)
        take_z(at, 1)
        ready(prior, 1)
        attend(prior, 1, 0)

        @pl.when(turn == 1)
        def _():
            query_copy.wait_recv()

        attend(prior, 0, 1)
        attend(prior, 1, 1)
        return carried

    lax.fori_loop(1, planes, one_turn, 0)
    last = place(planes - 1)
    ready(last, 0)
    attend(last, 0, 1)
    ready(last, 1)
    attend(last, 1, 1)
    part_out[...] = (weighted[1] / totals[1]).astype(jnp.bfloat16)
    stats_out[0:1, :] = maxima[1]
    stats_out[1:2, :] = totals[1]
    part_copy.start()
    stats_copy.start()
    attend(last, 0, 0)
    attend(last, 1, 0)
    loads[5].wait()
    stats_copy.wait_recv()
    highest = jnp.maximum(maxima[0], stats_in[0:1, :])
    fading_own = jnp.exp2((maxima[0] - highest) * scale)
    counted = stats_in[1:2, :] * jnp.exp2((stats_in[0:1, :] - highest) * scale)
    everything = totals[0] * fading_own + counted
    part_copy.wait_recv()
    shared = (weighted[0] * fading_own + part_in[...].astype(jnp.float32) * counted) / everything
    attended = jnp.concatenate(
        [shared[:, h * rows_q : (h + 1) * rows_q].T for h in range(heads)], axis=1
    ).astype(jnp.bfloat16)
    for h in range(heads):
        held[h * rows_q : (h + 1) * rows_q, :] = attended[:, h * head : (h + 1) * head]

    def product(slot):
        rows = jnp.concatenate(
            [
                held[pl.ds(pl.multiple_of(h * rows_q + slot * rows_t, rows_t), rows_t), :]
                for h in range(heads)
            ],
            axis=1,
        )
        return jnp.dot(rows, out_w[...], preferred_element_type=jnp.float32)

    sends = []
    for n, peer in enumerate((tp_xy, tp_x, tp_y)):
        outgoing[n] = product(peer).astype(jnp.bfloat16)
        copy = remote(outgoing.at[n], incoming.at[n], out_send.at[n], out_recv.at[n], (sp, peer))
        copy.start()
        sends.append(copy)
    mine = product(tp)
    for copy in (target_x, target_y, target_relay, query_copy, part_copy, stats_copy):
        copy.wait_send()

    y_copy(tp).wait_send()

    def drain(at, carried):
        for n in range(2):
            along_z(at, n, lambda copy: copy.wait_send())
            d_copy(at, n).wait_send()
        return carried

    lax.fori_loop(0, planes, drain, 0)
    for copy in sends:
        copy.wait_recv()
    update[...] = mine + (
        incoming[0].astype(jnp.float32)
        + incoming[1].astype(jnp.float32)
        + incoming[2].astype(jnp.float32)
    )
    for copy in sends:
        copy.wait_send()


def fused_body(
    n_sp,
    n_tp,
    target,
    source,
    target_gain,
    source_gain,
    query_weight,
    key_matrix,
    value_matrix,
    query_gain,
    key_gain,
    out_weight,
):
    rows_t, width = target.shape
    rows_s = source.shape[0]
    planes = n_sp // CORES
    heads = query_gain.shape[0]
    lanes = heads * n_tp * rows_t
    bf16, f32 = jnp.bfloat16, jnp.float32
    dma = pltpu.SemaphoreType.DMA
    any_spec = pl.BlockSpec(memory_space=pl.ANY)
    vmem_spec = pl.BlockSpec(memory_space=pltpu.VMEM)
    update = pl.pallas_call(
        functools.partial(fused_kernel, n_sp, n_tp),
        out_shape=jax.ShapeDtypeStruct((rows_t, width), f32),
        in_specs=[
            any_spec,
            any_spec,
            vmem_spec,
            vmem_spec,
            any_spec,
            any_spec,
            any_spec,
            vmem_spec,
            vmem_spec,
            any_spec,
        ],
        out_specs=vmem_spec,
        scratch_shapes=[
            pltpu.VMEM(target.shape, bf16),
            pltpu.VMEM(source.shape, bf16),
            pltpu.VMEM(query_weight.shape, bf16),
            pltpu.VMEM(key_matrix.shape, bf16),
            pltpu.VMEM(value_matrix.shape, bf16),
            pltpu.VMEM(out_weight.shape, bf16),
            pltpu.VMEM((n_tp, rows_t, width), bf16),
            pltpu.VMEM((2, lanes, HEAD_SIZE), bf16),
            pltpu.VMEM((planes, n_tp, CORES, rows_s, 2 * HEAD_SIZE), bf16),
            pltpu.VMEM((rows_s, 2 * HEAD_SIZE), bf16),
            pltpu.VMEM((2, 1, lanes), f32),
            pltpu.VMEM((2, 1, lanes), f32),
            pltpu.VMEM((2, HEAD_SIZE, lanes), f32),
            pltpu.VMEM((lanes, HEAD_SIZE), bf16),
            pltpu.VMEM((HEAD_SIZE, lanes), bf16),
            pltpu.VMEM((HEAD_SIZE, lanes), bf16),
            pltpu.VMEM((2, lanes), f32),
            pltpu.VMEM((2, lanes), f32),
            pltpu.VMEM((3, rows_t, width), bf16),
            pltpu.VMEM((3, rows_t, width), bf16),
            dma((6,)),
            dma((3,)),
            dma((3,)),
            dma((2, 2, planes)),
            dma((2, planes)),
            dma((1,)),
            dma((1,)),
            dma((3,)),
            dma((3,)),
            dma((2, planes)),
            dma((2, planes)),
            dma((3,)),
            dma((3,)),
        ],
        compiler_params=pltpu.CompilerParams(collective_id=0, has_side_effects=True),
    )(
        target,
        source,
        target_gain.reshape(1, -1),
        source_gain.reshape(1, -1),
        query_weight,
        key_matrix,
        value_matrix,
        query_gain,
        key_gain,
        out_weight,
    )
    return (target.astype(f32) + update).astype(bf16)


def solution(mesh):
    sp, tp = mesh.shape["sp"], mesh.shape["tp"]
    fits = tp == 2 * KEY_VALUE_HEADS and sp % CORES == 0 and sp > CORES
    return jax.shard_map(
        functools.partial(fused_body, sp, tp) if fits else body,
        mesh=mesh,
        in_specs=(
            P(("sp", "tp"), None),
            P(("sp", "tp"), None),
            P(),
            P(),
            P(None, "tp"),
            P(),
            P(),
            P("tp", None),
            P(),
            P("tp", None),
        ),
        out_specs=P(("sp", "tp"), None),
        check_vma=False,
    )
```

```python
import functools
import math

import jax
import jax.numpy as jnp
from jax import lax
from jax.experimental import pallas as pl
from jax.experimental.pallas import tpu as pltpu
from jax.sharding import PartitionSpec as P

KEY_VALUE_HEADS = 2
HEAD_SIZE = 128


EPSILON = 1e-06


def normed(values_in, gain):
    return (
        values_in
        * lax.rsqrt(jnp.mean(values_in * values_in, axis=-1, keepdims=True) + EPSILON)
        * gain
    )


def softmax_step(running, scores, seg_values, form):
    maxima, totals, weighted = running
    new_maxima = jnp.maximum(maxima, jnp.max(scores, axis=-1))
    fading = jnp.exp(maxima - new_maxima)
    weights = jnp.exp(scores - new_maxima[..., None])
    totals = totals * fading + jnp.sum(weights, axis=-1)
    weighted = weighted * fading[..., None] + jnp.einsum(
        form, weights.astype(jnp.bfloat16), seg_values, preferred_element_type=jnp.float32
    )
    return (new_maxima, totals, weighted)


def in_blocks(advance, running, segment, own_rows, limit):
    length = segment[0].shape[0]
    shards = length // own_rows
    widest = max(own_rows, limit)
    per_block = max(
        [
            number
            for number in range(1, shards + 1)
            if shards % number == 0 and own_rows * number <= widest
        ]
    )
    blocks = shards // per_block
    shaped = tuple(
        (member.reshape((blocks, own_rows * per_block) + member.shape[1:]) for member in segment)
    )

    def one_turn(carried, portion):
        return (advance(carried, portion), None)

    return lax.scan(one_turn, running, shaped)[0]


def body(
    target,
    source,
    target_gain,
    source_gain,
    query_weight,
    key_matrix,
    value_matrix,
    query_gain,
    key_gain,
    out_weight,
):
    local_heads = query_weight.shape[1] // HEAD_SIZE
    score_scale = 1.0 / math.sqrt(HEAD_SIZE)
    target_normed = normed(target.astype(jnp.float32), target_gain).astype(jnp.bfloat16)
    segment = lax.all_gather(target_normed, "tp", axis=0, tiled=True)
    raw_queries = jnp.dot(segment, query_weight, preferred_element_type=jnp.float32)
    shaped = raw_queries.reshape(segment.shape[0], local_heads, HEAD_SIZE)
    query_vectors = normed(shaped, query_gain).astype(jnp.bfloat16)
    block_rows = query_vectors.shape[0]
    normed_source_rows = normed(source.astype(jnp.float32), source_gain).astype(jnp.bfloat16)
    unnormed_keys = jnp.dot(
        normed_source_rows, key_matrix, preferred_element_type=jnp.float32
    ).reshape(source.shape[0], KEY_VALUE_HEADS, HEAD_SIZE)
    key_rows = normed(unnormed_keys, key_gain).astype(jnp.bfloat16)
    value_vectors = (
        jnp.dot(normed_source_rows, value_matrix, preferred_element_type=jnp.float32)
        .astype(jnp.bfloat16)
        .reshape(source.shape[0], KEY_VALUE_HEADS, HEAD_SIZE)
    )
    each_head_view = lax.axis_size("tp") // KEY_VALUE_HEADS
    sent_keys = jnp.repeat(key_rows, each_head_view, axis=1)
    sent_values = jnp.repeat(value_vectors, each_head_view, axis=1)
    head_keys, head_values = (
        lax.all_to_all(sent_keys, "tp", split_axis=1, concat_axis=0, tiled=True),
        lax.all_to_all(sent_values, "tp", split_axis=1, concat_axis=0, tiled=True),
    )
    head_keys = head_keys.reshape(-1, HEAD_SIZE)
    head_values = head_values.reshape(-1, HEAD_SIZE)
    own_rows = head_keys.shape[0]
    small_shape = (block_rows, local_heads)
    initial = (
        jnp.full(small_shape, -1e30, jnp.float32),
        jnp.zeros(small_shape, jnp.float32),
        jnp.zeros(small_shape + (HEAD_SIZE,), jnp.float32),
    )

    def advance(carried, portion):
        scores = (
            jnp.einsum("rhd,nd->rhn", query_vectors, portion[0], preferred_element_type=jnp.float32)
            * score_scale
        )
        return softmax_step(carried, scores, portion[1], "rhn,nd->rhd")

    maxima, totals, weighted = in_blocks(
        advance,
        initial,
        (
            lax.all_gather(head_keys, "sp", axis=0, tiled=True),
            lax.all_gather(head_values, "sp", axis=0, tiled=True),
        ),
        own_rows,
        1024,
    )
    attended = (
        (weighted / totals[..., None])
        .astype(jnp.bfloat16)
        .reshape(block_rows, local_heads * HEAD_SIZE)
    )
    portion = attended
    update = lax.psum_scatter(
        jnp.dot(portion, out_weight, preferred_element_type=jnp.float32).astype(jnp.bfloat16),
        "tp",
        scatter_dimension=0,
        tiled=True,
    ).astype(jnp.float32)
    return (target.astype(jnp.float32) + update).astype(jnp.bfloat16)


MESH = pl.DeviceIdType.MESH
CORES = 2


def fused_kernel(
    n_sp,
    n_tp,
    target_hbm,
    source_hbm,
    target_gain,
    source_gain,
    query_hbm,
    key_hbm,
    value_hbm,
    query_gain,
    key_gain,
    out_hbm,
    update,
    target_in,
    source_in,
    query_w,
    key_w,
    value_w,
    out_w,
    targets,
    queries,
    pairs,
    foreign,
    maxima,
    totals,
    weighted,
    held,
    part_out,
    part_in,
    stats_out,
    stats_in,
    outgoing,
    incoming,
    load_sem,
    target_send,
    target_recv,
    z_send,
    z_recv,
    y_send,
    y_recv,
    x_send,
    x_recv,
    d_send,
    d_recv,
    out_send,
    out_recv,
):
    planes = n_sp // CORES
    sp = lax.axis_index("sp")
    tp = lax.axis_index("tp")
    z, core = sp // CORES, sp % CORES
    y, x = tp // 2, tp % 2
    tp_x = y * 2 + (1 - x)
    tp_y = (1 - y) * 2 + x
    tp_xy = (1 - y) * 2 + (1 - x)
    mate = z * CORES + (1 - core)
    above, below = sp + CORES, sp - CORES
    head = HEAD_SIZE
    rows_t = target_in.shape[0]
    rows_s = source_in.shape[0]
    heads = query_gain.shape[0]
    rows_q = n_tp * rows_t

    loads = [
        pltpu.make_async_copy(a, b, load_sem.at[n])
        for n, (a, b) in enumerate(
            (
                (target_hbm, target_in),
                (source_hbm, source_in),
                (key_hbm, key_w),
                (value_hbm, value_w),
                (query_hbm, query_w),
                (out_hbm, out_w),
            )
        )
    ]
    for load in loads:
        load.start()

    barrier = pltpu.get_barrier_semaphore()
    for peer in ((sp, tp_x), (sp, tp_y), (sp, tp_xy), (mate, tp)):
        pl.semaphore_signal(barrier, inc=1, device_id=peer, device_id_type=MESH)

    @pl.when(z > 0)
    def _():
        pl.semaphore_signal(barrier, inc=1, device_id=(below, tp), device_id_type=MESH)

    @pl.when(z < planes - 1)
    def _():
        pl.semaphore_signal(barrier, inc=1, device_id=(above, tp), device_id_type=MESH)

    def remote(src, dst, send, recv, peer):
        return pltpu.make_async_remote_copy(
            src_ref=src,
            dst_ref=dst,
            send_sem=send,
            recv_sem=recv,
            device_id=peer,
            device_id_type=MESH,
        )

    loads[0].wait()
    targets[tp] = normed(target_in[...].astype(jnp.float32), target_gain[...]).astype(jnp.bfloat16)

    pl.semaphore_wait(barrier, 4 + jnp.minimum(z, 1) + jnp.minimum(planes - 1 - z, 1))

    def target_copy(slot, n, peer):
        return remote(
            targets.at[slot], targets.at[slot], target_send.at[n], target_recv.at[n], peer
        )

    target_x = target_copy(tp, 0, (sp, tp_x))
    target_y = target_copy(tp, 1, (sp, tp_y))
    target_relay = target_copy(tp_x, 2, (sp, tp_y))
    target_x.start()
    target_y.start()

    loads[1].wait()
    source_normed = normed(source_in[...].astype(jnp.float32), source_gain[...]).astype(
        jnp.bfloat16
    )
    loads[2].wait()
    raw_keys = jnp.dot(source_normed, key_w[...], preferred_element_type=jnp.float32)
    loads[3].wait()
    raw_values = jnp.dot(source_normed, value_w[...], preferred_element_type=jnp.float32)

    made = []
    for h in range(KEY_VALUE_HEADS):
        cut = slice(h * head, (h + 1) * head)
        keys = normed(raw_keys[:, cut], key_gain[h : h + 1, :]).astype(jnp.bfloat16)
        made.append((keys, raw_values[:, cut].astype(jnp.bfloat16)))
    mine_zero = y == 0
    for part in range(2):
        cut = slice(part * head, (part + 1) * head)
        pairs[z, tp, core, :, cut] = jnp.where(mine_zero, made[0][part], made[1][part])
        foreign[:, cut] = jnp.where(mine_zero, made[1][part], made[0][part])

    def z_copy(at, n, up):
        block = pairs.at[at, slots[n], core]
        way = 0 if up else 1
        peer = (above if up else below, tp)
        return remote(block, block, z_send.at[n, way, at], z_recv.at[n, at], peer)

    def along_z(at, n, act):
        @pl.when(jnp.logical_and(at <= z, z < planes - 1))
        def _():
            act(z_copy(at, n, True))

        @pl.when(jnp.logical_and(at >= z, z > 0))
        def _():
            act(z_copy(at, n, False))

    def y_copy(slot):
        return remote(foreign, pairs.at[z, slot, core], y_send.at[0], y_recv.at[0], (sp, tp_y))

    def x_copy(src, dst, n):
        return remote(src, dst, x_send.at[n], x_recv.at[n], (sp, tp_x))

    query_copy = x_copy(queries.at[0], queries.at[1], 0)
    part_copy = x_copy(part_out, part_in, 1)
    stats_copy = x_copy(stats_out, stats_in, 2)
    slots = (tp, tp_y)

    def d_copy(at, n):
        block = pairs.at[at, slots[n], core]
        return remote(block, block, d_send.at[n, at], d_recv.at[n, at], (mate, tp))

    def d_arrival(at, n):
        block = pairs.at[at, slots[n], 1 - core]
        return remote(block, block, d_send.at[n, at], d_recv.at[n, at], (mate, tp))

    def place(turn):
        other = planes - 1 - z
        near = jnp.minimum(z, other)
        step = (turn + 1) // 2
        signed = z + step * (1 - 2 * (turn % 2))
        far = jnp.where(z < other, turn, planes - 1 - turn)
        return jnp.where(turn <= 2 * near, signed, far)

    def launch(at, n):
        along_z(at, n, lambda copy: copy.start())
        d_copy(at, n).start()

    def take_z(at, n):
        z_copy(at, n, True).wait_recv()
        launch(at, n)

    scale = math.log2(math.e) / math.sqrt(head)

    def ready(at, n):
        d_arrival(at, n).wait_recv()

    def attend(at, n, half):
        both = pairs[at, slots[n]].reshape(CORES * rows_s, 2 * head)
        scores = lax.dot_general(
            both[:, :head],
            queries[half],
            (((1,), (1,)), ((), ())),
            preferred_element_type=jnp.float32,
        )
        before = maxima[half]
        after = jnp.maximum(before, jnp.max(scores, axis=0, keepdims=True))
        weights = jnp.exp2((scores - after) * scale)
        fading = jnp.exp2((before - after) * scale)
        maxima[half] = after
        totals[half] = totals[half] * fading + jnp.sum(weights, axis=0, keepdims=True)
        weighted[half] = weighted[half] * fading + lax.dot_general(
            both[:, head:],
            weights.astype(jnp.bfloat16),
            (((0,), (0,)), ((), ())),
            preferred_element_type=jnp.float32,
        )

    y_copy(tp).start()
    launch(z, 0)

    maxima[...] = jnp.full(maxima.shape, -1e30, jnp.float32)
    totals[...] = jnp.zeros(totals.shape, jnp.float32)
    weighted[...] = jnp.zeros(weighted.shape, jnp.float32)

    target_copy(tp_x, 0, (sp, tp_x)).wait_recv()
    target_relay.start()
    target_copy(tp_y, 1, (sp, tp_y)).wait_recv()
    y_copy(tp_y).wait_recv()
    launch(z, 1)
    target_copy(tp_xy, 2, (sp, tp_y)).wait_recv()
    loads[4].wait()
    all_targets = targets[...].reshape(rows_q, targets.shape[2])
    raw = jnp.dot(all_targets, query_w[...], preferred_element_type=jnp.float32)
    for h in range(heads):
        queries[0, h * rows_q : (h + 1) * rows_q, :] = normed(
            raw[:, h * head : (h + 1) * head], query_gain[h : h + 1, :]
        ).astype(jnp.bfloat16)

    query_copy.start()

    def one_turn(turn, carried):
        at = place(turn)
        prior = place(turn - 1)
        take_z(at, 0)
        ready(prior, 0)
        attend(prior, 0, 0)
        take_z(at, 1)
        ready(prior, 1)
        attend(prior, 1, 0)

        @pl.when(turn == 2)
        def _():
            query_copy.wait_recv()
            attend(z, 0, 1)
            attend(z, 1, 1)

        @pl.when(turn >= 2)
        def _():
            attend(prior, 0, 1)
            attend(prior, 1, 1)

        return carried

    lax.fori_loop(1, planes, one_turn, 0)
    last = place(planes - 1)
    ready(last, 0)
    attend(last, 0, 1)
    ready(last, 1)
    attend(last, 1, 1)
    part_out[...] = (weighted[1] / totals[1]).astype(jnp.bfloat16)
    stats_out[0:1, :] = maxima[1]
    stats_out[1:2, :] = totals[1]
    part_copy.start()
    stats_copy.start()
    attend(last, 0, 0)
    attend(last, 1, 0)
    loads[5].wait()
    stats_copy.wait_recv()
    highest = jnp.maximum(maxima[0], stats_in[0:1, :])
    fading_own = jnp.exp2((maxima[0] - highest) * scale)
    counted = stats_in[1:2, :] * jnp.exp2((stats_in[0:1, :] - highest) * scale)
    everything = totals[0] * fading_own + counted
    part_copy.wait_recv()
    shared = (weighted[0] * fading_own + part_in[...].astype(jnp.float32) * counted) / everything
    attended = jnp.concatenate(
        [shared[:, h * rows_q : (h + 1) * rows_q].T for h in range(heads)], axis=1
    ).astype(jnp.bfloat16)
    for h in range(heads):
        held[h * rows_q : (h + 1) * rows_q, :] = attended[:, h * head : (h + 1) * head]

    def product(slot):
        rows = jnp.concatenate(
            [
                held[pl.ds(pl.multiple_of(h * rows_q + slot * rows_t, rows_t), rows_t), :]
                for h in range(heads)
            ],
            axis=1,
        )
        return jnp.dot(rows, out_w[...], preferred_element_type=jnp.float32)

    sends = []
    for n, peer in enumerate((tp_xy, tp_x, tp_y)):
        outgoing[n] = product(peer).astype(jnp.bfloat16)
        copy = remote(outgoing.at[n], incoming.at[n], out_send.at[n], out_recv.at[n], (sp, peer))
        copy.start()
        sends.append(copy)
    mine = product(tp)
    for copy in (target_x, target_y, target_relay, query_copy, part_copy, stats_copy):
        copy.wait_send()

    y_copy(tp).wait_send()

    def drain(at, carried):
        for n in range(2):
            along_z(at, n, lambda copy: copy.wait_send())
            d_copy(at, n).wait_send()
        return carried

    lax.fori_loop(0, planes, drain, 0)
    for copy in sends:
        copy.wait_recv()
    update[...] = mine + (
        incoming[0].astype(jnp.float32)
        + incoming[1].astype(jnp.float32)
        + incoming[2].astype(jnp.float32)
    )
    for copy in sends:
        copy.wait_send()


def fused_body(
    n_sp,
    n_tp,
    target,
    source,
    target_gain,
    source_gain,
    query_weight,
    key_matrix,
    value_matrix,
    query_gain,
    key_gain,
    out_weight,
):
    rows_t, width = target.shape
    rows_s = source.shape[0]
    planes = n_sp // CORES
    heads = query_gain.shape[0]
    lanes = heads * n_tp * rows_t
    bf16, f32 = jnp.bfloat16, jnp.float32
    dma = pltpu.SemaphoreType.DMA
    any_spec = pl.BlockSpec(memory_space=pl.ANY)
    vmem_spec = pl.BlockSpec(memory_space=pltpu.VMEM)
    update = pl.pallas_call(
        functools.partial(fused_kernel, n_sp, n_tp),
        out_shape=jax.ShapeDtypeStruct((rows_t, width), f32),
        in_specs=[
            any_spec,
            any_spec,
            vmem_spec,
            vmem_spec,
            any_spec,
            any_spec,
            any_spec,
            vmem_spec,
            vmem_spec,
            any_spec,
        ],
        out_specs=vmem_spec,
        scratch_shapes=[
            pltpu.VMEM(target.shape, bf16),
            pltpu.VMEM(source.shape, bf16),
            pltpu.VMEM(query_weight.shape, bf16),
            pltpu.VMEM(key_matrix.shape, bf16),
            pltpu.VMEM(value_matrix.shape, bf16),
            pltpu.VMEM(out_weight.shape, bf16),
            pltpu.VMEM((n_tp, rows_t, width), bf16),
            pltpu.VMEM((2, lanes, HEAD_SIZE), bf16),
            pltpu.VMEM((planes, n_tp, CORES, rows_s, 2 * HEAD_SIZE), bf16),
            pltpu.VMEM((rows_s, 2 * HEAD_SIZE), bf16),
            pltpu.VMEM((2, 1, lanes), f32),
            pltpu.VMEM((2, 1, lanes), f32),
            pltpu.VMEM((2, HEAD_SIZE, lanes), f32),
            pltpu.VMEM((lanes, HEAD_SIZE), bf16),
            pltpu.VMEM((HEAD_SIZE, lanes), bf16),
            pltpu.VMEM((HEAD_SIZE, lanes), bf16),
            pltpu.VMEM((2, lanes), f32),
            pltpu.VMEM((2, lanes), f32),
            pltpu.VMEM((3, rows_t, width), bf16),
            pltpu.VMEM((3, rows_t, width), bf16),
            dma((6,)),
            dma((3,)),
            dma((3,)),
            dma((2, 2, planes)),
            dma((2, planes)),
            dma((1,)),
            dma((1,)),
            dma((3,)),
            dma((3,)),
            dma((2, planes)),
            dma((2, planes)),
            dma((3,)),
            dma((3,)),
        ],
        compiler_params=pltpu.CompilerParams(collective_id=0, has_side_effects=True),
    )(
        target,
        source,
        target_gain.reshape(1, -1),
        source_gain.reshape(1, -1),
        query_weight,
        key_matrix,
        value_matrix,
        query_gain,
        key_gain,
        out_weight,
    )
    return (target.astype(f32) + update).astype(bf16)


def solution(mesh):
    sp, tp = mesh.shape["sp"], mesh.shape["tp"]
    fits = tp == 2 * KEY_VALUE_HEADS and sp % CORES == 0 and sp > 2 * CORES
    return jax.shard_map(
        functools.partial(fused_body, sp, tp) if fits else body,
        mesh=mesh,
        in_specs=(
            P(("sp", "tp"), None),
            P(("sp", "tp"), None),
            P(),
            P(),
            P(None, "tp"),
            P(),
            P(),
            P("tp", None),
            P(),
            P("tp", None),
        ),
        out_specs=P(("sp", "tp"), None),
        check_vma=False,
    )
```
